32 devices in a mesh: sp: 16 (over z, y, core), tp: 2 (over x).
Axes of the slice: x: 2, y: 2, z: 4, core: 2. Of those that a mesh axis runs over, the one named last changes fastest.
Arguments:
- tokens: bfloat16 [16384, 2048], P('sp'), may hold values from -6 to 6
- norm_gain: float32 [2048], replicated, may hold values from 0.1 to 1.9
- w_query: bfloat16 [2048, 512], P(None, 'tp'), may hold values from -0.79549513 to 0.79549513
- w_key: bfloat16 [2048, 128], P('sp'), may hold values from -0.79549513 to 0.79549513
- w_value: bfloat16 [2048, 128], P('sp'), may hold values from -0.125 to 0.125
- w_pool_in: bfloat16 [2048, 512], P(None, 'tp'), may hold values from -0.125 to 0.125
- sink_logit: float32 [8], P('tp'), may hold values from 3 to 7
- pool_scale: float32 [512], P('tp'), may hold values from 0.05 to 0.5
- w_out: bfloat16 [1024, 2048], P('tp', 'sp'), may hold values from -0.75 to 0.75
Outputs:
- mixed_out: bfloat16 [16384, 2048], P(('sp', 'tp'))
The draws below stay inside these ranges and needn't reach their ends.
All inputs are finite; a program needn't handle non-finite values.
Results may differ from the reference program's by a relative error of at most 0.03.
The reference program's roundings to bfloat16 on the way (of `normed`, `query`, `key`, `value`, `pool_in`, `weights`, `attended` and `pooled`) count: a program that leaves them out, or rounds other values in their place, can miss the bound.
Values may be sent and summed in bfloat16 or wider, within the bound.
A program may use at most 64 MiB of HBM per device.

```python
import math
import jax
import jax.numpy as jnp
from jax import lax

D = 2048
HEAD = 64
QH = 8
KVH = 2
POOL_CH = 128
POOL_W = 512
WINDOW = 128
QB = 128
SEQ = 16384


def projection_draw(key, shape):
    values = jax.random.truncated_normal(key, -6.0, 6.0, shape, jnp.float32) * D ** (-0.5)
    return values.astype(jnp.bfloat16)


def draw_w_query(key, part):
    return projection_draw(jax.random.fold_in(key, 11), (D, QH * HEAD))


def draw_w_key(key, part):
    return projection_draw(jax.random.fold_in(key, 23), (D, KVH * HEAD))


def level_of(key, dims, pieces, smallest, top_value):
    level = 1.0
    for dim, parts in pieces:
        steps = jax.random.uniform(jax.random.fold_in(jax.random.fold_in(key, 6), dim), (parts,), jnp.float32, smallest / len(pieces), top_value / len(pieces))
        level = level * jnp.repeat(jnp.exp(steps), dims[dim] // parts).reshape((-1,) + (1,) * (len(dims) - 1 - dim))
    return level


def centred(rng, dims, scale, reach, pieces=(), kind=jnp.bfloat16):
    entries = scale * jax.random.normal(rng, dims, jnp.float32)
    if pieces:
        entries = entries * level_of(rng, dims, pieces, -0.22, 0.18)
    return jnp.clip(entries, -reach, reach).astype(kind)


def setup_inputs(seed: int = 0) -> dict:
    seeds = jax.random.split(jax.random.key(seed), 10)
    tokens = centred(seeds[0], (SEQ, D), 1.0, 6.0, ((0, 16),))
    norm_gain = jnp.clip(1.0 + 0.18 * jax.random.normal(seeds[1], (D,), jnp.float32), 0.1, 1.9)
    w_query = draw_w_query(jax.random.fold_in(seeds[9], 71), 0)
    w_key = draw_w_key(jax.random.fold_in(seeds[9], 71), 0)
    w_value = centred(seeds[4], (D, KVH * HEAD), D ** -0.5, 0.125, ((0, 16),))
    w_pool_in = centred(seeds[5], (D, POOL_W), D ** -0.5, 0.125, ((1, 2),))
    sink_logit = jnp.clip(3.0 + 4.0 * jax.random.uniform(seeds[6], (QH,), jnp.float32) ** level_of(seeds[6], (QH,), ((0, 2),), -0.2, 0.2), 3.0, 7.0)
    pool_scale = jnp.clip(jnp.exp(math.log(0.5) - 2.3025851 * jax.random.uniform(seeds[7], (POOL_W,), jnp.float32) ** level_of(seeds[7], (POOL_W,), ((0, 2),), -0.2, 0.2)), 0.05, 0.5)
    w_out = centred(seeds[8], (QH * HEAD + POOL_W, D), (4.0 * (QH * HEAD + POOL_W) ** -0.5), 0.75, ((0, 2), (1, 16)))
    return {"tokens": tokens, "norm_gain": norm_gain, "w_query": w_query, "w_key": w_key, "w_value": w_value, "w_pool_in": w_pool_in, "sink_logit": sink_logit, "pool_scale": pool_scale, "w_out": w_out}


NEG_BIG = -1e+30
POOL_SPANS = (2, 4, 8, 16)

def layer_normed(tokens, norm_gain):
    values = tokens.astype(jnp.float32)
    center = lax.optimization_barrier(jnp.mean(values, axis=-1, keepdims=True))
    spread = lax.optimization_barrier(jnp.mean(jnp.square(values - center), axis=-1, keepdims=True))
    return ((values - center) * lax.rsqrt(spread + 1e-06) * norm_gain).astype(jnp.bfloat16)

def rotate(values, positions):
    half = HEAD // 2
    inverse = 10000.0 ** (-jnp.arange(half, dtype=jnp.float32) / half)
    angles = positions[:, None] * inverse[None, :]
    cosine = jnp.cos(angles)[:, None, :]
    sine = jnp.sin(angles)[:, None, :]
    first = values[..., :half]
    second = values[..., half:]
    return jnp.concatenate([first * cosine - second * sine, first * sine + second * cosine], axis=-1)

def reference(tokens, norm_gain, w_query, w_key, w_value, w_pool_in, sink_logit, pool_scale, w_out):
    length = tokens.shape[0]
    group = QH // KVH
    normed = layer_normed(tokens, norm_gain)
    positions = jnp.arange(length).astype(jnp.float32)
    query = rotate(jnp.dot(normed, w_query, preferred_element_type=jnp.float32).reshape(length, QH, HEAD), positions).astype(jnp.bfloat16)
    key = rotate(jnp.dot(normed, w_key, preferred_element_type=jnp.float32).reshape(length, KVH, HEAD), positions).astype(jnp.bfloat16)
    value = jnp.dot(normed, w_value, preferred_element_type=jnp.float32).astype(jnp.bfloat16).reshape(length, KVH, HEAD)
    pool_in = jnp.dot(normed, w_pool_in, preferred_element_type=jnp.float32).astype(jnp.bfloat16)
    key_padded = jnp.pad(key, ((WINDOW, WINDOW), (0, 0), (0, 0)))
    value_padded = jnp.pad(value, ((WINDOW, WINDOW), (0, 0), (0, 0)))
    span = QB + 2 * WINDOW
    sink_grid = sink_logit.reshape(KVH, group)[:, :, None, None]

    def attend(start):
        queries = lax.dynamic_slice_in_dim(query, start, QB, 0).reshape(QB, KVH, group, HEAD)
        keys = lax.dynamic_slice_in_dim(key_padded, start, span, 0)
        values = lax.dynamic_slice_in_dim(value_padded, start, span, 0)
        scores = jnp.einsum('ikgd,jkd->kgij', queries.astype(jnp.float32), keys.astype(jnp.float32)) * HEAD ** (-0.5)
        query_pos = start + jnp.arange(QB).astype(jnp.int32)
        key_pos = start - WINDOW + jnp.arange(span).astype(jnp.int32)
        valid = (jnp.abs(query_pos[:, None] - key_pos[None, :]) <= WINDOW) & (key_pos[None, :] >= 0) & (key_pos[None, :] < length)
        scores = jnp.where(valid, scores, NEG_BIG)
        highest = jnp.maximum(lax.optimization_barrier(jnp.max(scores, axis=-1, keepdims=True)), sink_grid)
        expo = jnp.where(valid, jnp.exp(scores - highest), 0.0)
        total = lax.optimization_barrier(jnp.sum(expo, axis=-1, keepdims=True)) + jnp.exp(sink_grid - highest)
        weights = (expo / total).astype(jnp.bfloat16)
        result = jnp.einsum('kgij,jkd->ikgd', weights.astype(jnp.float32), values.astype(jnp.float32))
        return result.reshape(QB, QH * HEAD).astype(jnp.bfloat16)
    starts = (jnp.arange(length // QB) * QB).astype(jnp.int32)
    attended = lax.map(attend, starts).reshape(length, QH * HEAD)
    pool_vals = pool_in.astype(jnp.float32)
    running = jnp.pad(jnp.cumsum(pool_vals, axis=0), ((1, 0), (0, 0)))
    where_at = jnp.arange(length).astype(jnp.int32)
    means = []
    for index, width in enumerate(POOL_SPANS):
        lower = jnp.clip(where_at - width // 2, 0, length)
        upper = jnp.clip(where_at + width // 2, 0, length)
        block = running[:, index * POOL_CH:(index + 1) * POOL_CH]
        means.append((block[upper] - block[lower]) / (upper - lower).astype(jnp.float32)[:, None])
    pooled = ((jnp.concatenate(means, axis=1) - pool_vals) * pool_scale).astype(jnp.bfloat16)
    joined = jnp.concatenate([attended, pooled], axis=1)
    return jnp.dot(joined, w_out, preferred_element_type=jnp.float32).astype(jnp.bfloat16)
```

```python
import functools

import jax
import jax.numpy as jnp
from jax import lax
from jax.experimental import pallas as pl
from jax.experimental.pallas import tpu as pltpu
from jax.sharding import PartitionSpec as P

HEAD = 64
QH = 8
KVH = 2
POOL_CH = 128
WINDOW = 128
QB = 128


NEG_BIG = -1e30
POOL_SPANS = (2, 4, 8, 16)


def extended(block, sides, width):
    for axis, dim in sides:
        count = lax.axis_size(axis)
        forward = [(i, i + 1) for i in range(count - 1)]
        backward = [(target, source) for source, target in forward]
        low = lax.ppermute(
            lax.slice_in_dim(block, block.shape[dim] - width, None, axis=dim), axis, forward
        )
        high = lax.ppermute(lax.slice_in_dim(block, 0, width, axis=dim), axis, backward)
        block = jnp.concatenate([low, block, high], axis=dim)
    return block


def layer_normed(tokens, norm_gain):
    values = tokens.astype(jnp.float32)
    center = jnp.mean(values, axis=-1, keepdims=True)
    spread = jnp.mean(jnp.square(values - center), axis=-1, keepdims=True)
    return ((values - center) * lax.rsqrt(spread + 1e-06) * norm_gain).astype(jnp.bfloat16)


def rotate(values, positions):
    half = HEAD // 2
    inverse = 10000.0 ** (-jnp.arange(half, dtype=jnp.float32) / half)
    angles = positions[:, None] * inverse[None, :]
    cosine = jnp.cos(angles)[:, None, :]
    sine = jnp.sin(angles)[:, None, :]
    first = values[..., :half]
    second = values[..., half:]
    return jnp.concatenate(
        [first * cosine - second * sine, first * sine + second * cosine], axis=-1
    )


def plain_body(tokens, norm_gain, w_query, w_key, w_value, w_pool_in, sink_logit, pool_scale, w_out):
    local_rows = tokens.shape[0]
    seq_total = local_rows * lax.axis_size("sp")
    offset = lax.axis_index("sp") * local_rows
    tp_place = lax.axis_index("tp")
    local_heads = w_query.shape[1] // HEAD
    local_pool = w_pool_in.shape[1]
    reach = POOL_SPANS[-1] // 2
    normed = layer_normed(tokens, norm_gain)
    positions = (offset + jnp.arange(local_rows)).astype(jnp.float32)
    query = rotate(
        jnp.dot(normed, w_query, preferred_element_type=jnp.float32).reshape(
            local_rows, local_heads, HEAD
        ),
        positions,
    ).astype(jnp.bfloat16)
    key_head = tp_place * local_heads // (QH // KVH)
    key_cols = lax.dynamic_slice_in_dim(w_key, key_head * HEAD, HEAD, 1)
    value_cols = lax.dynamic_slice_in_dim(w_value, key_head * HEAD, HEAD, 1)
    key_sum = jnp.dot(
        normed,
        lax.all_gather(key_cols, "sp", axis=0, tiled=True),
        preferred_element_type=jnp.float32,
    )
    value_sum = jnp.dot(
        normed,
        lax.all_gather(value_cols, "sp", axis=0, tiled=True),
        preferred_element_type=jnp.float32,
    )
    key = rotate(key_sum[:, None, :], positions)[:, 0, :].astype(jnp.bfloat16)
    value = value_sum.astype(jnp.bfloat16)
    key_value = jnp.concatenate([key, value], axis=1)
    pool_in = jnp.dot(normed, w_pool_in, preferred_element_type=jnp.float32).astype(jnp.bfloat16)
    widened = extended(jnp.concatenate([key_value, pool_in], axis=1), (("sp", 0),), WINDOW)
    kv_wide = widened[:, : 2 * HEAD]
    pool_wide = widened[WINDOW - reach : WINDOW + local_rows + reach, 2 * HEAD :]
    span = QB + 2 * WINDOW
    sink_here = sink_logit[:, None, None]
    results = []
    for block in range(local_rows // QB):
        queries = query[block * QB : (block + 1) * QB]
        keys = kv_wide[block * QB : block * QB + span, :HEAD]
        values = kv_wide[block * QB : block * QB + span, HEAD:]
        scores = jnp.einsum(
            "ihd,jd->hij", queries, keys, preferred_element_type=jnp.float32
        ) * HEAD ** (-0.5)
        query_pos = offset + block * QB + jnp.arange(QB)
        key_pos = offset + block * QB - WINDOW + jnp.arange(span)
        valid = (
            (jnp.abs(query_pos[:, None] - key_pos[None, :]) <= WINDOW)
            & (key_pos[None, :] >= 0)
            & (key_pos[None, :] < seq_total)
        )
        scores = jnp.where(valid, scores, NEG_BIG)
        highest = jnp.maximum(jnp.max(scores, axis=-1, keepdims=True), sink_here)
        expo = jnp.where(valid, jnp.exp(scores - highest), 0.0)
        total = jnp.sum(expo, axis=-1, keepdims=True) + jnp.exp(sink_here - highest)
        weights = (expo / total).astype(jnp.bfloat16)
        result = jnp.einsum("hij,jd->ihd", weights, values, preferred_element_type=jnp.float32)
        results.append(result.reshape(QB, local_heads * HEAD).astype(jnp.bfloat16))
    attended = jnp.concatenate(results, axis=0)
    pool_vals = pool_wide.astype(jnp.float32)
    window_sum = pool_vals
    global_pos = offset + jnp.arange(local_rows)
    channel = tp_place * local_pool + jnp.arange(local_pool)
    window_group = channel // POOL_CH
    measured = jnp.zeros((local_rows, local_pool), jnp.float32)
    stride = 1
    for index, width in enumerate(POOL_SPANS):
        window_sum = window_sum[:-stride] + window_sum[stride:]
        stride = width
        sums = window_sum[reach - width // 2 : reach - width // 2 + local_rows]
        counted = (
            jnp.minimum(global_pos + width // 2, seq_total)
            - jnp.maximum(global_pos - width // 2, 0)
        ).astype(jnp.float32)
        measured = measured + jnp.where(
            window_group[None, :] == index, sums / counted[:, None], 0.0
        )
    pooled = ((measured - pool_vals[reach : reach + local_rows]) * pool_scale).astype(jnp.bfloat16)
    attended_rows, pooled_rows = (
        lax.all_to_all(attended, "tp", split_axis=0, concat_axis=1, tiled=True),
        lax.all_to_all(pooled, "tp", split_axis=0, concat_axis=1, tiled=True),
    )
    joined = jnp.concatenate([attended_rows, pooled_rows], axis=1)
    out_rows_all = lax.all_gather(w_out, "tp", axis=0, tiled=True)
    projected = jnp.dot(
        joined,
        lax.all_gather(out_rows_all, "sp", axis=1, tiled=True),
        preferred_element_type=jnp.float32,
    )
    return projected.astype(jnp.bfloat16)


LANES = 128
CHUNK = 256
MESH = pl.DeviceIdType.MESH


def rope_tables(offset, rows):
    half = HEAD // 2
    inverse = 10000.0 ** (-jnp.arange(half, dtype=jnp.float32) / half)
    inverse = jnp.tile(inverse, LANES // half)[None, :]
    sign = jnp.where(jnp.arange(LANES) % HEAD < half, -1.0, 1.0)[None, :]
    inner = jnp.arange(QB, dtype=jnp.float32)[:, None] * inverse
    starts = (offset + QB * jnp.arange(rows // QB)).astype(jnp.float32)[:, None] * inverse
    return jnp.cos(inner), jnp.sin(inner) * sign, jnp.cos(starts), jnp.sin(starts) * sign


def mixer_kernel(
    places, tokens, gain, w_query, kv_block, w_pool, sink, scale, w_out, cos_in, sin_in, cos_at, sin_at,
    out,
    tok, normed, wq, wp, kvw, wfull, qs, kv, pool, pool_send, att_send, joined, out_v,
    tok_sem, own_sem, out_sem, kv_send, kv_recv, kvf_send, wx_send, wx_recv, wo_send, wo_recv,
    wf_send, wp_send, halo_send, halo_recv, ex_send, ex_recv,
):
    S, T = places
    Z = S // 4
    s = lax.axis_index("sp")
    t = lax.axis_index("tp")
    rows = tokens.shape[0]
    width = tokens.shape[1]
    blocks = rows // QB
    hb = blocks // 2
    chunks = rows // CHUNK
    local_heads = w_query.shape[1] // HEAD
    groups = w_query.shape[1] // LANES
    pgroups = w_pool.shape[1] // LANES
    reach = POOL_SPANS[-1] // 2
    offset = s * rows
    total_rows = S * rows
    c = s % 2
    y = (s // 2) % 2
    z = s // 4
    quad = s % 4
    partner = s + 1 - 2 * c
    yflip = s + 2 - 4 * y
    after = (s + 1) % S
    before = (s + S - 1) % S
    cross = 1 - t
    hops = sorted(range(1, Z), key=lambda d: (min(d, Z - d), d))

    def zmate(d, base):
        return ((z + d) % Z) * 4 + base % 4

    def remote(a, b, send, recv, to_s, to_t):
        return pltpu.make_async_remote_copy(
            src_ref=a, dst_ref=b, send_sem=send, recv_sem=recv,
            device_id={"sp": to_s, "tp": to_t}, device_id_type=MESH,
        )

    same_core = [zmate(d, s) for d in hops] + [zmate(d, yflip) for d in range(Z)]

    tok_copies = [
        pltpu.make_async_copy(
            tokens.at[pl.ds(i * CHUNK, CHUNK)], tok.at[pl.ds(i * CHUNK, CHUNK)], tok_sem.at[i]
        )
        for i in range(chunks)
    ]
    tok_copies[0].start()
    own_copies = [
        pltpu.make_async_copy(w_query, wq, own_sem.at[0]),
        pltpu.make_async_copy(w_pool, wp, own_sem.at[1]),
        pltpu.make_async_copy(kv_block, kvw.at[s], own_sem.at[2]),
        pltpu.make_async_copy(w_out, wfull.at[s, t], own_sem.at[3]),
    ]
    for copy in own_copies:
        copy.start()
    for copy in tok_copies[1:]:
        copy.start()

    barrier = pltpu.get_barrier_semaphore()
    greet = [(b, t) for b in same_core + [after, before]] + [(s, cross)]
    for to_s, to_t in greet:
        pl.semaphore_signal(barrier, inc=1, device_id={"sp": to_s, "tp": to_t}, device_id_type=MESH)
    pl.semaphore_wait(barrier, len(greet))

    kv_copies = [
        remote(kv_block, kvw.at[s], kv_send.at[i], kv_recv.at[s], b, t)
        for i, b in enumerate(same_core)
    ]
    for copy in kv_copies:
        copy.start()
    x_copy = remote(w_out, wfull.at[s, t], wx_send, wx_recv, s, cross)
    x_copy.start()
    x_in = remote(w_out, wfull.at[s, cross], wx_send, wx_recv, s, cross)

    kv_forward = [
        remote(kvw.at[b], kvw.at[b], kvf_send.at[i], kv_recv.at[b], partner, t)
        for i, b in enumerate([s] + same_core)
    ]
    wo_first = [
        remote(wfull.at[s], wfull.at[s], wo_send.at[i], wo_recv.at[s], b, t)
        for i, b in enumerate([yflip] + [zmate(d, s) for d in hops] + [partner])
    ]
    wo_z = []
    for i, d in enumerate(hops):
        b = zmate(d, s)
        wo_z.append([
            remote(wfull.at[b], wfull.at[b], wf_send.at[2 * i + k], wo_recv.at[b], to, t)
            for k, to in enumerate([yflip, partner])
        ])
    wo_y = []
    for i, d in enumerate([0] + hops):
        b = zmate(d, yflip)
        wo_y.append(remote(wfull.at[b], wfull.at[b], wp_send.at[i], wo_recv.at[b], partner, t))

    def forward_z(i):
        wo_z[i][0].wait_recv()
        wo_z[i][0].start()
        wo_z[i][1].start()

    def forward_y(i):
        wo_y[i].wait_recv()
        wo_y[i].start()

    lane = lax.broadcasted_iota(jnp.int32, (QB, LANES), 1)
    low_half = lane < HEAD
    first_half = lane % HEAD < HEAD // 2

    def rotated(values, b):
        ca = cos_at[pl.ds(b, 1), :]
        sa = sin_at[pl.ds(b, 1), :]
        ci = cos_in[...]
        si = sin_in[...]
        cosine = ca * ci - sa * si
        sine = sa * ci + ca * si
        swapped = jnp.where(
            first_half,
            pltpu.roll(values, LANES - HEAD // 2, 1),
            pltpu.roll(values, HEAD // 2, 1),
        )
        return values * cosine + swapped * sine

    own_copies[0].wait()
    own_copies[1].wait()
    LN = 32

    def project(i, carry):
        base = pl.multiple_of(i * CHUNK, CHUNK)
        pltpu.make_async_copy(
            tokens.at[pl.ds(base, CHUNK)], tok.at[pl.ds(base, CHUNK)], tok_sem.at[i]
        ).wait()

        def norm(r, carry):
            at = pl.multiple_of(base + r * LN, LN)
            values = tok[pl.ds(at, LN), :].astype(jnp.float32)
            center = jnp.sum(values, axis=1, keepdims=True) * (1.0 / width)
            moved = values - center
            spread = jnp.sum(moved * moved, axis=1, keepdims=True) * (1.0 / width)
            normed[pl.ds(at, LN), :] = (moved * lax.rsqrt(spread + 1e-06) * gain[...]).astype(
                jnp.bfloat16
            )
            return carry

        lax.fori_loop(0, CHUNK // LN, norm, 0, unroll=2)
        part = normed[pl.ds(base, CHUNK), :]
        query = jnp.dot(part, wq[...], preferred_element_type=jnp.float32)
        for k in range(CHUNK // QB):
            b = i * (CHUNK // QB) + k
            for g in range(groups):
                turned = rotated(query[k * QB:(k + 1) * QB, g * LANES:(g + 1) * LANES], b) * HEAD ** (-0.5)
                qs[b, pl.ds(2 * g * QB, QB), :] = jnp.where(low_half, turned, 0.0).astype(jnp.bfloat16)
                qs[b, pl.ds((2 * g + 1) * QB, QB), :] = jnp.where(
                    low_half, pltpu.roll(turned, HEAD, 1), 0.0
                ).astype(jnp.bfloat16)
        mixed = jnp.dot(part, wp[...], preferred_element_type=jnp.float32)
        pool[pl.ds(pl.multiple_of(reach + base, 8), CHUNK), :] = mixed.astype(jnp.bfloat16).astype(jnp.float32)

        @pl.when(i == 1)
        def _():
            own_copies[3].wait()
            x_in.wait_recv()
            for copy in wo_first:
                copy.start()

        @pl.when(i == 2)
        def _():
            own_copies[2].wait()
            for copy in kv_forward[1:]:
                copy.wait_recv()
            for copy in kv_forward:
                copy.start()
        return carry

    lax.fori_loop(0, chunks, project, 0)

    halo_pool = [
        remote(pool.at[pl.ds(rows, reach)], pool.at[pl.ds(0, reach)], halo_send.at[0], halo_recv.at[0], after, t),
        remote(pool.at[pl.ds(reach, reach)], pool.at[pl.ds(rows + reach, reach)], halo_send.at[1], halo_recv.at[1], before, t),
    ]
    halo_kv = [
        remote(kv.at[pl.ds(rows, WINDOW)], kv.at[pl.ds(0, WINDOW)], halo_send.at[2], halo_recv.at[2], after, t),
        remote(kv.at[pl.ds(WINDOW, WINDOW)], kv.at[pl.ds(rows + WINDOW, WINDOW)], halo_send.at[3], halo_recv.at[3], before, t),
    ]

    for b in [partner] + [zmate(d, partner) for d in hops] + [zmate(d, partner + 2 - 4 * y) for d in range(Z)]:
        remote(kvw.at[b], kvw.at[b], kvf_send.at[0], kv_recv.at[b], partner, t).wait_recv()

    def key_value(j, carry):
        i = jnp.where(j == 0, 0, jnp.where(j == 1, chunks - 1, j - 1))
        base = pl.multiple_of(i * CHUNK, CHUNK)
        both = jnp.dot(
            normed[pl.ds(base, CHUNK), :], kvw[...].reshape(width, LANES), preferred_element_type=jnp.float32
        )
        for k in range(CHUNK // QB):
            piece = both[k * QB:(k + 1) * QB, :]
            turned = rotated(piece, i * (CHUNK // QB) + k)
            kv[pl.ds(pl.multiple_of(WINDOW + base + k * QB, QB), QB), :] = jnp.where(
                low_half, turned, piece
            ).astype(jnp.bfloat16)

        @pl.when(j == 0)
        def _():
            for copy in halo_pool:
                copy.start()

        @pl.when(j == 2)
        def _():
            for copy in halo_kv:
                copy.start()
        return carry

    lax.fori_loop(0, chunks, key_value, 0)

    for copy in halo_pool:
        copy.wait_recv()

    @pl.when(s == 0)
    def _():
        pool[0:reach, :] = jnp.zeros((reach, pool.shape[1]), jnp.float32)

    @pl.when(s == S - 1)
    def _():
        pool[rows + reach:rows + 2 * reach, :] = jnp.zeros((reach, pool.shape[1]), jnp.float32)

    def pooled(b, g):
        cols = slice(g * LANES, (g + 1) * LANES)
        length = QB + 2 * reach
        values = pool[pl.ds(pl.multiple_of(b * QB, QB), length), cols]
        index = (t * (pgroups * LANES) + g * LANES) // POOL_CH
        running = values
        stride = 1
        picked = jnp.zeros((QB, LANES), jnp.float32)
        wide = 0
        for k, span in enumerate(POOL_SPANS):
            running = running + pltpu.roll(running, length - stride, 0)
            stride = span
            shift = reach - span // 2
            sums = (pltpu.roll(running, length - shift, 0) if shift else running)[:QB]
            picked = jnp.where(index == k, sums, picked)
            wide = jnp.where(index == k, span // 2, wide)
        pos = offset + b * QB + lax.broadcasted_iota(jnp.int32, (QB, LANES), 0)
        counted = (jnp.minimum(pos + wide, total_rows) - jnp.maximum(pos - wide, 0)).astype(jnp.float32)
        return ((picked / counted - values[reach:reach + QB]) * scale[:, cols]).astype(jnp.bfloat16)

    def pool_other(i, carry):
        for g in range(pgroups):
            pool_send[pl.ds(pl.multiple_of(i * QB, QB), QB), g * LANES:(g + 1) * LANES] = pooled(cross * hb + i, g)
        return carry

    def pool_own(i, carry):
        for g in range(pgroups):
            joined[T + t, pl.ds(pl.multiple_of(i * QB, QB), QB), g * LANES:(g + 1) * LANES] = pooled(t * hb + i, g)
        return carry

    ex_pool = remote(pool_send, joined.at[T + t], ex_send.at[0], ex_recv.at[0], s, cross)
    ex_att = remote(att_send, joined.at[t], ex_send.at[1], ex_recv.at[1], s, cross)
    lax.fori_loop(0, hb, pool_other, 0)
    lax.fori_loop(0, hb, pool_own, 0)
    ex_pool.start()
    for i in range(min(2, len(hops))):
        forward_z(i)

    span = QB + 2 * WINDOW
    row_id = lax.broadcasted_iota(jnp.int32, (QB, span), 0)
    col_id = lax.broadcasted_iota(jnp.int32, (QB, span), 1)

    def attend(b):
        context = kv[pl.ds(pl.multiple_of(b * QB, QB), span), :]
        scores = lax.dot_general(
            qs[b], context, (((1,), (1,)), ((), ())), preferred_element_type=jnp.float32
        )
        start = offset + b * QB
        lowest = jnp.maximum(row_id, WINDOW - start)
        highest_col = jnp.minimum(row_id + 2 * WINDOW, total_rows - 1 - start + WINDOW)
        valid = (col_id >= lowest) & (col_id <= highest_col)
        expos = []
        norms = []
        for h in range(local_heads):
            part = jnp.where(valid, scores[h * QB:(h + 1) * QB], NEG_BIG)
            top = jnp.maximum(jnp.max(part, axis=1, keepdims=True), sink[h])
            expo = jnp.exp(part - top)
            norms.append(1.0 / (jnp.sum(expo, axis=1, keepdims=True) + jnp.exp(sink[h] - top)))
            expos.append(expo.astype(jnp.bfloat16))
        result = jnp.dot(jnp.concatenate(expos, axis=0), context, preferred_element_type=jnp.float32)
        heads = [result[h * QB:(h + 1) * QB] * norms[h] for h in range(local_heads)]
        return [
            jnp.where(low_half, pltpu.roll(heads[2 * g], HEAD, 1), heads[2 * g + 1]).astype(jnp.bfloat16)
            for g in range(groups)
        ]

    def attend_other(i, carry):
        @pl.when(i == hb - 1)
        def _():
            halo_kv[0].wait_recv()
            halo_kv[1].wait_recv()
        b = jnp.where(t == 0, hb + i, hb - 1 - i)
        at = pl.multiple_of((b - cross * hb) * QB, QB)
        for g, value in enumerate(attend(b)):
            att_send[pl.ds(at, QB), g * LANES:(g + 1) * LANES] = value
        return carry

    def attend_own(i, carry):
        b = jnp.where(t == 0, hb - 1 - i, hb + i)
        at = pl.multiple_of((b - t * hb) * QB, QB)
        for g, value in enumerate(attend(b)):
            joined[t, pl.ds(at, QB), g * LANES:(g + 1) * LANES] = value

        @pl.when(i == 0)
        def _():
            ex_att.start()
        return carry

    lax.fori_loop(0, hb, attend_other, 0)
    forward_y(0)
    for i in range(2, len(hops)):
        forward_z(i)
    lax.fori_loop(0, hb, attend_own, 0)
    for i in range(1, Z):
        forward_y(i)

    remote(pool_send, joined.at[T + cross], ex_send.at[0], ex_recv.at[0], s, cross).wait_recv()
    remote(att_send, joined.at[cross], ex_send.at[1], ex_recv.at[1], s, cross).wait_recv()
    for base_place in (partner, partner + 2 - 4 * y):
        for d in [0] + hops:
            b = zmate(d, base_place)
            remote(wfull.at[b], wfull.at[b], wp_send.at[0], wo_recv.at[b], partner, t).wait_recv()

    def out_copy(n):
        return pltpu.make_async_copy(
            out_v.at[n], out.at[:, pl.ds(pl.multiple_of(n * 2 * LANES, 2 * LANES), 2 * LANES)], out_sem.at[n]
        )

    def finish(n, carry):
        left = jnp.concatenate([joined[k] for k in range(2 * T)], axis=1)
        right = jnp.concatenate(
            [wfull[2 * n].reshape(left.shape[1], LANES), wfull[2 * n + 1].reshape(left.shape[1], LANES)], axis=1
        )
        out_v[n] = jnp.dot(left, right, preferred_element_type=jnp.float32).astype(jnp.bfloat16)
        out_copy(n).start()
        return carry

    lax.fori_loop(0, S // 2, finish, 0)
    for copy in kv_copies + [x_copy] + kv_forward + wo_first + wo_y + halo_pool + halo_kv + [ex_pool, ex_att]:
        copy.wait_send()
    for pair in wo_z:
        for copy in pair:
            copy.wait_send()
    for n in range(S // 2):
        out_copy(n).wait()


def body(mesh, tokens, norm_gain, w_query, w_key, w_value, w_pool_in, sink_logit, pool_scale, w_out):
    S = lax.axis_size("sp")
    T = lax.axis_size("tp")
    rows, width = tokens.shape
    local_heads = w_query.shape[1] // HEAD
    fits = (
        S % 4 == 0 and S > 4 and T == 2
        and w_out.shape[1] == LANES and w_key.shape[0] == LANES
        and w_query.shape[1] % LANES == 0 and w_pool_in.shape[1] % LANES == 0
        and w_query.shape[1] == w_pool_in.shape[1]
        and local_heads == QH // KVH and rows % (2 * CHUNK) == 0
    )
    if not fits:
        return plain_body(
            tokens, norm_gain, w_query, w_key, w_value, w_pool_in, sink_logit, pool_scale, w_out
        )
    place = lax.axis_index("tp")
    key_head = place * local_heads // (QH // KVH)
    kv_block = jnp.concatenate(
        [
            lax.dynamic_slice_in_dim(w_key, key_head * HEAD, HEAD, 1),
            lax.dynamic_slice_in_dim(w_value, key_head * HEAD, HEAD, 1),
        ],
        axis=1,
    )
    tables = rope_tables(lax.axis_index("sp") * rows, rows)
    blocks = rows // QB
    half = rows // T
    Z = S // 4
    reach = POOL_SPANS[-1] // 2
    wide = w_query.shape[1]
    vmem = pl.BlockSpec(memory_space=pltpu.VMEM)
    smem = pl.BlockSpec(memory_space=pltpu.SMEM)
    hbm = pl.BlockSpec(memory_space=pl.ANY)
    dma = pltpu.SemaphoreType.DMA
    bf = jnp.bfloat16
    return pl.pallas_call(
        functools.partial(mixer_kernel, (S, T)),
        out_shape=jax.ShapeDtypeStruct((half, S * w_out.shape[1]), bf),
        in_specs=[hbm, vmem, hbm, hbm, hbm, smem, vmem, hbm, vmem, vmem, vmem, vmem],
        out_specs=hbm,
        scratch_shapes=[
            pltpu.VMEM((rows, width), bf),
            pltpu.VMEM((rows, width), bf),
            pltpu.VMEM(w_query.shape, bf),
            pltpu.VMEM(w_pool_in.shape, bf),
            pltpu.VMEM((S, LANES, LANES), bf),
            pltpu.VMEM((S, T) + w_out.shape, bf),
            pltpu.VMEM((blocks, local_heads * QB, LANES), bf),
            pltpu.VMEM((rows + 2 * WINDOW, LANES), bf),
            pltpu.VMEM((rows + 2 * reach, wide), jnp.float32),
            pltpu.VMEM((half, wide), bf),
            pltpu.VMEM((half, wide), bf),
            pltpu.VMEM((2 * T, half, wide), bf),
            pltpu.VMEM((S // 2, half, 2 * LANES), bf),
            dma((rows // CHUNK,)),
            dma((4,)),
            dma((S // 2,)),
            dma((S // 2 - 1,)),
            dma((S,)),
            dma((S // 2,)),
            dma(()),
            dma(()),
            dma((Z + 1,)),
            dma((S,)),
            dma((2 * (Z - 1),)),
            dma((Z,)),
            dma((4,)),
            dma((4,)),
            dma((2,)),
            dma((2,)),
        ],
        compiler_params=pltpu.CompilerParams(
            collective_id=0, has_side_effects=True, vmem_limit_bytes=44 * 1024 * 1024
        ),
    )(
        tokens, norm_gain[None, :], w_query, kv_block, w_pool_in, sink_logit, pool_scale[None, :], w_out, *tables
    )


def solution(mesh):
    in_specs = (
        P("sp", None),
        P(),
        P(None, "tp"),
        P("sp", None),
        P("sp", None),
        P(None, "tp"),
        P("tp"),
        P("tp"),
        P("tp", "sp"),
    )
    out_specs = P(("sp", "tp"), None)
    return jax.shard_map(functools.partial(body, mesh), mesh=mesh, in_specs=in_specs, out_specs=out_specs, check_vma=False)
```

```python
import functools

import jax
import jax.numpy as jnp
from jax import lax
from jax.experimental import pallas as pl
from jax.experimental.pallas import tpu as pltpu
from jax.sharding import PartitionSpec as P

HEAD = 64
QH = 8
KVH = 2
POOL_CH = 128
WINDOW = 128
QB = 128


NEG_BIG = -1e30
POOL_SPANS = (2, 4, 8, 16)


def extended(block, sides, width):
    for axis, dim in sides:
        count = lax.axis_size(axis)
        forward = [(i, i + 1) for i in range(count - 1)]
        backward = [(target, source) for source, target in forward]
        low = lax.ppermute(
            lax.slice_in_dim(block, block.shape[dim] - width, None, axis=dim), axis, forward
        )
        high = lax.ppermute(lax.slice_in_dim(block, 0, width, axis=dim), axis, backward)
        block = jnp.concatenate([low, block, high], axis=dim)
    return block


def layer_normed(tokens, norm_gain):
    values = tokens.astype(jnp.float32)
    center = jnp.mean(values, axis=-1, keepdims=True)
    spread = jnp.mean(jnp.square(values - center), axis=-1, keepdims=True)
    return ((values - center) * lax.rsqrt(spread + 1e-06) * norm_gain).astype(jnp.bfloat16)


def rotate(values, positions):
    half = HEAD // 2
    inverse = 10000.0 ** (-jnp.arange(half, dtype=jnp.float32) / half)
    angles = positions[:, None] * inverse[None, :]
    cosine = jnp.cos(angles)[:, None, :]
    sine = jnp.sin(angles)[:, None, :]
    first = values[..., :half]
    second = values[..., half:]
    return jnp.concatenate(
        [first * cosine - second * sine, first * sine + second * cosine], axis=-1
    )


def plain_body(tokens, norm_gain, w_query, w_key, w_value, w_pool_in, sink_logit, pool_scale, w_out):
    local_rows = tokens.shape[0]
    seq_total = local_rows * lax.axis_size("sp")
    offset = lax.axis_index("sp") * local_rows
    tp_place = lax.axis_index("tp")
    local_heads = w_query.shape[1] // HEAD
    local_pool = w_pool_in.shape[1]
    reach = POOL_SPANS[-1] // 2
    normed = layer_normed(tokens, norm_gain)
    positions = (offset + jnp.arange(local_rows)).astype(jnp.float32)
    query = rotate(
        jnp.dot(normed, w_query, preferred_element_type=jnp.float32).reshape(
            local_rows, local_heads, HEAD
        ),
        positions,
    ).astype(jnp.bfloat16)
    key_head = tp_place * local_heads // (QH // KVH)
    key_cols = lax.dynamic_slice_in_dim(w_key, key_head * HEAD, HEAD, 1)
    value_cols = lax.dynamic_slice_in_dim(w_value, key_head * HEAD, HEAD, 1)
    key_sum = jnp.dot(
        normed,
        lax.all_gather(key_cols, "sp", axis=0, tiled=True),
        preferred_element_type=jnp.float32,
    )
    value_sum = jnp.dot(
        normed,
        lax.all_gather(value_cols, "sp", axis=0, tiled=True),
        preferred_element_type=jnp.float32,
    )
    key = rotate(key_sum[:, None, :], positions)[:, 0, :].astype(jnp.bfloat16)
    value = value_sum.astype(jnp.bfloat16)
    key_value = jnp.concatenate([key, value], axis=1)
    pool_in = jnp.dot(normed, w_pool_in, preferred_element_type=jnp.float32).astype(jnp.bfloat16)
    widened = extended(jnp.concatenate([key_value, pool_in], axis=1), (("sp", 0),), WINDOW)
    kv_wide = widened[:, : 2 * HEAD]
    pool_wide = widened[WINDOW - reach : WINDOW + local_rows + reach, 2 * HEAD :]
    span = QB + 2 * WINDOW
    sink_here = sink_logit[:, None, None]
    results = []
    for block in range(local_rows // QB):
        queries = query[block * QB : (block + 1) * QB]
        keys = kv_wide[block * QB : block * QB + span, :HEAD]
        values = kv_wide[block * QB : block * QB + span, HEAD:]
        scores = jnp.einsum(
            "ihd,jd->hij", queries, keys, preferred_element_type=jnp.float32
        ) * HEAD ** (-0.5)
        query_pos = offset + block * QB + jnp.arange(QB)
        key_pos = offset + block * QB - WINDOW + jnp.arange(span)
        valid = (
            (jnp.abs(query_pos[:, None] - key_pos[None, :]) <= WINDOW)
            & (key_pos[None, :] >= 0)
            & (key_pos[None, :] < seq_total)
        )
        scores = jnp.where(valid, scores, NEG_BIG)
        highest = jnp.maximum(jnp.max(scores, axis=-1, keepdims=True), sink_here)
        expo = jnp.where(valid, jnp.exp(scores - highest), 0.0)
        total = jnp.sum(expo, axis=-1, keepdims=True) + jnp.exp(sink_here - highest)
        weights = (expo / total).astype(jnp.bfloat16)
        result = jnp.einsum("hij,jd->ihd", weights, values, preferred_element_type=jnp.float32)
        results.append(result.reshape(QB, local_heads * HEAD).astype(jnp.bfloat16))
    attended = jnp.concatenate(results, axis=0)
    pool_vals = pool_wide.astype(jnp.float32)
    window_sum = pool_vals
    global_pos = offset + jnp.arange(local_rows)
    channel = tp_place * local_pool + jnp.arange(local_pool)
    window_group = channel // POOL_CH
    measured = jnp.zeros((local_rows, local_pool), jnp.float32)
    stride = 1
    for index, width in enumerate(POOL_SPANS):
        window_sum = window_sum[:-stride] + window_sum[stride:]
        stride = width
        sums = window_sum[reach - width // 2 : reach - width // 2 + local_rows]
        counted = (
            jnp.minimum(global_pos + width // 2, seq_total)
            - jnp.maximum(global_pos - width // 2, 0)
        ).astype(jnp.float32)
        measured = measured + jnp.where(
            window_group[None, :] == index, sums / counted[:, None], 0.0
        )
    pooled = ((measured - pool_vals[reach : reach + local_rows]) * pool_scale).astype(jnp.bfloat16)
    attended_rows, pooled_rows = (
        lax.all_to_all(attended, "tp", split_axis=0, concat_axis=1, tiled=True),
        lax.all_to_all(pooled, "tp", split_axis=0, concat_axis=1, tiled=True),
    )
    joined = jnp.concatenate([attended_rows, pooled_rows], axis=1)
    out_rows_all = lax.all_gather(w_out, "tp", axis=0, tiled=True)
    projected = jnp.dot(
        joined,
        lax.all_gather(out_rows_all, "sp", axis=1, tiled=True),
        preferred_element_type=jnp.float32,
    )
    return projected.astype(jnp.bfloat16)


LANES = 128
CHUNK = 256
MESH = pl.DeviceIdType.MESH


def rope_tables(offset, rows):
    half = HEAD // 2
    inverse = 10000.0 ** (-jnp.arange(half, dtype=jnp.float32) / half)
    inverse = jnp.tile(inverse, LANES // half)[None, :]
    sign = jnp.where(jnp.arange(LANES) % HEAD < half, -1.0, 1.0)[None, :]
    inner = jnp.arange(QB, dtype=jnp.float32)[:, None] * inverse
    starts = (offset + QB * jnp.arange(rows // QB)).astype(jnp.float32)[:, None] * inverse
    return jnp.cos(inner), jnp.sin(inner) * sign, jnp.cos(starts), jnp.sin(starts) * sign


def mixer_kernel(
    places, tokens, gain, w_query, kv_block, w_pool, sink, scale, w_out, cos_in, sin_in, cos_at, sin_at,
    out,
    tok, normed, wq, wp, kvw, wfull, qs, kv, pool, pool_send, att_send, joined, out_v,
    tok_sem, own_sem, out_sem, kv_send, kv_recv, kvf_send, wx_send, wx_recv, wo_send, wo_recv,
    wf_send, wp_send, halo_send, halo_recv, ex_send, ex_recv,
):
    S, T = places
    Z = S // 4
    s = lax.axis_index("sp")
    t = lax.axis_index("tp")
    rows = tokens.shape[0]
    width = tokens.shape[1]
    blocks = rows // QB
    hb = blocks // 2
    chunks = rows // CHUNK
    local_heads = w_query.shape[1] // HEAD
    groups = w_query.shape[1] // LANES
    pgroups = w_pool.shape[1] // LANES
    reach = POOL_SPANS[-1] // 2
    offset = s * rows
    total_rows = S * rows
    c = s % 2
    y = (s // 2) % 2
    z = s // 4
    quad = s % 4
    partner = s + 1 - 2 * c
    yflip = s + 2 - 4 * y
    after = (s + 1) % S
    before = (s + S - 1) % S
    cross = 1 - t
    hops = sorted(range(1, Z), key=lambda d: (min(d, Z - d), d))

    def zmate(d, base):
        return ((z + d) % Z) * 4 + base % 4

    def remote(a, b, send, recv, to_s, to_t):
        return pltpu.make_async_remote_copy(
            src_ref=a, dst_ref=b, send_sem=send, recv_sem=recv,
            device_id={"sp": to_s, "tp": to_t}, device_id_type=MESH,
        )

    same_core = [zmate(d, s) for d in hops] + [zmate(d, yflip) for d in range(Z)]

    tok_copies = [
        pltpu.make_async_copy(
            tokens.at[pl.ds(i * CHUNK, CHUNK)], tok.at[pl.ds(i * CHUNK, CHUNK)], tok_sem.at[i]
        )
        for i in range(chunks)
    ]
    tok_copies[0].start()
    own_copies = [
        pltpu.make_async_copy(w_query, wq, own_sem.at[0]),
        pltpu.make_async_copy(w_pool, wp, own_sem.at[1]),
        pltpu.make_async_copy(kv_block, kvw.at[s], own_sem.at[2]),
        pltpu.make_async_copy(w_out, wfull.at[s, t], own_sem.at[3]),
    ]
    for copy in own_copies:
        copy.start()
    for copy in tok_copies[1:]:
        copy.start()

    barrier = pltpu.get_barrier_semaphore()
    greet = [(b, t) for b in same_core + [after, before]] + [(s, cross)]
    for to_s, to_t in greet:
        pl.semaphore_signal(barrier, inc=1, device_id={"sp": to_s, "tp": to_t}, device_id_type=MESH)
    pl.semaphore_wait(barrier, len(greet))

    kv_copies = [
        remote(kv_block, kvw.at[s], kv_send.at[i], kv_recv.at[s], b, t)
        for i, b in enumerate(same_core)
    ]
    for copy in kv_copies:
        copy.start()
    x_copy = remote(w_out, wfull.at[s, t], wx_send, wx_recv, s, cross)
    x_copy.start()
    x_in = remote(w_out, wfull.at[s, cross], wx_send, wx_recv, s, cross)

    kv_forward = [
        remote(kvw.at[b], kvw.at[b], kvf_send.at[i], kv_recv.at[b], partner, t)
        for i, b in enumerate([s] + same_core)
    ]
    wo_to = [zmate(d, s) for d in hops] + [yflip, partner]
    wo_own = [
        remote(w_out, wfull.at[s, t], wo_send.at[0, i], wo_recv.at[s, t], b, t)
        for i, b in enumerate(wo_to)
    ]
    wo_crossed = [
        remote(wfull.at[s, cross], wfull.at[s, cross], wo_send.at[1, i], wo_recv.at[s, cross], b, t)
        for i, b in enumerate(wo_to)
    ]
    for copy in wo_own:
        copy.start()

    def z_copies(i, k):
        b = zmate(hops[i], s)
        half = cross if k else t
        piece = wfull.at[b, half]
        return [
            remote(piece, piece, wf_send.at[k, 2 * i + j], wo_recv.at[b, half], to, t)
            for j, to in enumerate([yflip, partner])
        ]

    def y_copy(d, k):
        b = zmate(d, yflip)
        half = cross if k else t
        piece = wfull.at[b, half]
        return remote(piece, piece, wp_send.at[k, d], wo_recv.at[b, half], partner, t)

    def forward_z(i, k):
        copies = z_copies(i, k)
        copies[0].wait_recv()
        for copy in copies:
            copy.start()

    def forward_y(d, k):
        copy = y_copy(d, k)
        copy.wait_recv()
        copy.start()

    lane = lax.broadcasted_iota(jnp.int32, (QB, LANES), 1)
    low_half = lane < HEAD
    first_half = lane % HEAD < HEAD // 2

    def rotated(values, b):
        ca = cos_at[pl.ds(b, 1), :]
        sa = sin_at[pl.ds(b, 1), :]
        ci = cos_in[...]
        si = sin_in[...]
        cosine = ca * ci - sa * si
        sine = sa * ci + ca * si
        swapped = jnp.where(
            first_half,
            pltpu.roll(values, LANES - HEAD // 2, 1),
            pltpu.roll(values, HEAD // 2, 1),
        )
        return values * cosine + swapped * sine

    own_copies[0].wait()
    own_copies[1].wait()
    LN = 32

    def project(i, carry):
        base = pl.multiple_of(i * CHUNK, CHUNK)
        pltpu.make_async_copy(
            tokens.at[pl.ds(base, CHUNK)], tok.at[pl.ds(base, CHUNK)], tok_sem.at[i]
        ).wait()

        def norm(r, carry):
            at = pl.multiple_of(base + r * LN, LN)
            values = tok[pl.ds(at, LN), :].astype(jnp.float32)
            center = jnp.sum(values, axis=1, keepdims=True) * (1.0 / width)
            moved = values - center
            spread = jnp.sum(moved * moved, axis=1, keepdims=True) * (1.0 / width)
            normed[pl.ds(at, LN), :] = (moved * lax.rsqrt(spread + 1e-06) * gain[...]).astype(
                jnp.bfloat16
            )
            return carry

        lax.fori_loop(0, CHUNK // LN, norm, 0, unroll=2)
        part = normed[pl.ds(base, CHUNK), :]
        query = jnp.dot(part, wq[...], preferred_element_type=jnp.float32)
        for k in range(CHUNK // QB):
            b = i * (CHUNK // QB) + k
            for g in range(groups):
                turned = rotated(query[k * QB:(k + 1) * QB, g * LANES:(g + 1) * LANES], b) * HEAD ** (-0.5)
                qs[b, pl.ds(2 * g * QB, QB), :] = jnp.where(low_half, turned, 0.0).astype(jnp.bfloat16)
                qs[b, pl.ds((2 * g + 1) * QB, QB), :] = jnp.where(
                    low_half, pltpu.roll(turned, HEAD, 1), 0.0
                ).astype(jnp.bfloat16)
        mixed = jnp.dot(part, wp[...], preferred_element_type=jnp.float32)
        pool[pl.ds(pl.multiple_of(reach + base, 8), CHUNK), :] = mixed.astype(jnp.bfloat16).astype(jnp.float32)

        @pl.when(i == 0)
        def _():
            x_in.wait_recv()
            for copy in wo_crossed:
                copy.start()

        @pl.when(i == 2)
        def _():
            own_copies[2].wait()
            for copy in kv_forward[1:]:
                copy.wait_recv()
            for copy in kv_forward:
                copy.start()
        return carry

    lax.fori_loop(0, chunks, project, 0)

    halo_pool = [
        remote(pool.at[pl.ds(rows, reach)], pool.at[pl.ds(0, reach)], halo_send.at[0], halo_recv.at[0], after, t),
        remote(pool.at[pl.ds(reach, reach)], pool.at[pl.ds(rows + reach, reach)], halo_send.at[1], halo_recv.at[1], before, t),
    ]
    halo_kv = [
        remote(kv.at[pl.ds(rows, WINDOW)], kv.at[pl.ds(0, WINDOW)], halo_send.at[2], halo_recv.at[2], after, t),
        remote(kv.at[pl.ds(WINDOW, WINDOW)], kv.at[pl.ds(rows + WINDOW, WINDOW)], halo_send.at[3], halo_recv.at[3], before, t),
    ]

    for b in [partner] + [zmate(d, partner) for d in hops] + [zmate(d, partner + 2 - 4 * y) for d in range(Z)]:
        remote(kvw.at[b], kvw.at[b], kvf_send.at[0], kv_recv.at[b], partner, t).wait_recv()

    def key_value(j, carry):
        i = jnp.where(j == 0, 0, jnp.where(j == 1, chunks - 1, j - 1))
        base = pl.multiple_of(i * CHUNK, CHUNK)
        both = jnp.dot(
            normed[pl.ds(base, CHUNK), :], kvw[...].reshape(width, LANES), preferred_element_type=jnp.float32
        )
        for k in range(CHUNK // QB):
            piece = both[k * QB:(k + 1) * QB, :]
            turned = rotated(piece, i * (CHUNK // QB) + k)
            kv[pl.ds(pl.multiple_of(WINDOW + base + k * QB, QB), QB), :] = jnp.where(
                low_half, turned, piece
            ).astype(jnp.bfloat16)

        @pl.when(j == 0)
        def _():
            for copy in halo_pool:
                copy.start()

        @pl.when(j == 2)
        def _():
            for copy in halo_kv:
                copy.start()
        return carry

    lax.fori_loop(0, chunks, key_value, 0)

    for copy in halo_pool:
        copy.wait_recv()

    @pl.when(s == 0)
    def _():
        pool[0:reach, :] = jnp.zeros((reach, pool.shape[1]), jnp.float32)

    @pl.when(s == S - 1)
    def _():
        pool[rows + reach:rows + 2 * reach, :] = jnp.zeros((reach, pool.shape[1]), jnp.float32)

    def pooled(b, g):
        cols = slice(g * LANES, (g + 1) * LANES)
        length = QB + 2 * reach
        values = pool[pl.ds(pl.multiple_of(b * QB, QB), length), cols]
        index = (t * (pgroups * LANES) + g * LANES) // POOL_CH
        running = values
        stride = 1
        picked = jnp.zeros((QB, LANES), jnp.float32)
        wide = 0
        for k, span in enumerate(POOL_SPANS):
            running = running + pltpu.roll(running, length - stride, 0)
            stride = span
            shift = reach - span // 2
            sums = (pltpu.roll(running, length - shift, 0) if shift else running)[:QB]
            picked = jnp.where(index == k, sums, picked)
            wide = jnp.where(index == k, span // 2, wide)
        pos = offset + b * QB + lax.broadcasted_iota(jnp.int32, (QB, LANES), 0)
        counted = (jnp.minimum(pos + wide, total_rows) - jnp.maximum(pos - wide, 0)).astype(jnp.float32)
        return ((picked / counted - values[reach:reach + QB]) * scale[:, cols]).astype(jnp.bfloat16)

    def pool_other(i, carry):
        for g in range(pgroups):
            pool_send[pl.ds(pl.multiple_of(i * QB, QB), QB), g * LANES:(g + 1) * LANES] = pooled(cross * hb + i, g)
        return carry

    def pool_own(i, carry):
        for g in range(pgroups):
            joined[T + t, pl.ds(pl.multiple_of(i * QB, QB), QB), g * LANES:(g + 1) * LANES] = pooled(t * hb + i, g)
        return carry

    ex_pool = remote(pool_send, joined.at[T + t], ex_send.at[0], ex_recv.at[0], s, cross)
    ex_att = remote(att_send, joined.at[t], ex_send.at[1], ex_recv.at[1], s, cross)
    lax.fori_loop(0, hb, pool_other, 0)
    lax.fori_loop(0, hb, pool_own, 0)
    ex_pool.start()
    for i in range(len(hops)):
        forward_z(i, 0)

    span = QB + 2 * WINDOW
    row_id = lax.broadcasted_iota(jnp.int32, (QB, span), 0)
    col_id = lax.broadcasted_iota(jnp.int32, (QB, span), 1)

    def attend(b):
        context = kv[pl.ds(pl.multiple_of(b * QB, QB), span), :]
        scores = lax.dot_general(
            qs[b], context, (((1,), (1,)), ((), ())), preferred_element_type=jnp.float32
        )
        start = offset + b * QB
        lowest = jnp.maximum(row_id, WINDOW - start)
        highest_col = jnp.minimum(row_id + 2 * WINDOW, total_rows - 1 - start + WINDOW)
        valid = (col_id >= lowest) & (col_id <= highest_col)
        expos = []
        norms = []
        for h in range(local_heads):
            part = jnp.where(valid, scores[h * QB:(h + 1) * QB], NEG_BIG)
            top = jnp.maximum(jnp.max(part, axis=1, keepdims=True), sink[h])
            expo = jnp.exp(part - top)
            norms.append(1.0 / (jnp.sum(expo, axis=1, keepdims=True) + jnp.exp(sink[h] - top)))
            expos.append(expo.astype(jnp.bfloat16))
        result = jnp.dot(jnp.concatenate(expos, axis=0), context, preferred_element_type=jnp.float32)
        heads = [result[h * QB:(h + 1) * QB] * norms[h] for h in range(local_heads)]
        return [
            jnp.where(low_half, pltpu.roll(heads[2 * g], HEAD, 1), heads[2 * g + 1]).astype(jnp.bfloat16)
            for g in range(groups)
        ]

    def attend_other(i, carry):
        @pl.when(i == hb - 1)
        def _():
            halo_kv[0].wait_recv()
            halo_kv[1].wait_recv()
        b = jnp.where(t == 0, hb + i, hb - 1 - i)
        at = pl.multiple_of((b - cross * hb) * QB, QB)
        for g, value in enumerate(attend(b)):
            att_send[pl.ds(at, QB), g * LANES:(g + 1) * LANES] = value
        return carry

    def attend_own(i, carry):
        b = jnp.where(t == 0, hb - 1 - i, hb + i)
        at = pl.multiple_of((b - t * hb) * QB, QB)
        for g, value in enumerate(attend(b)):
            joined[t, pl.ds(at, QB), g * LANES:(g + 1) * LANES] = value

        @pl.when(i == 0)
        def _():
            ex_att.start()
        return carry

    lax.fori_loop(0, hb, attend_other, 0)
    lax.fori_loop(0, hb, attend_own, 0)
    for i in range(len(hops)):
        forward_z(i, 1)
    for d in range(Z):
        forward_y(d, 0)
    own_copies[3].wait()

    remote(pool_send, joined.at[T + cross], ex_send.at[0], ex_recv.at[0], s, cross).wait_recv()
    remote(att_send, joined.at[cross], ex_send.at[1], ex_recv.at[1], s, cross).wait_recv()
    def out_copy(n):
        return pltpu.make_async_copy(
            out_v.at[n], out.at[:, pl.ds(pl.multiple_of(n * 2 * LANES, 2 * LANES), 2 * LANES)], out_sem.at[n]
        )

    def finish(j, carry):
        over = j // Z
        @pl.when(over == 0)
        def _():
            forward_y(j, 1)
        side = y + over - 2 * y * over
        n = ((z + j) % Z) * 2 + side
        for half in range(T):
            piece = wfull.at[2 * n + 1 - c, half]
            remote(piece, piece, wp_send.at[0, 0], wo_recv.at[2 * n + 1 - c, half], partner, t).wait_recv()
        left = jnp.concatenate([joined[k] for k in range(2 * T)], axis=1)
        right = jnp.concatenate(
            [wfull[2 * n].reshape(left.shape[1], LANES), wfull[2 * n + 1].reshape(left.shape[1], LANES)], axis=1
        )
        out_v[n] = jnp.dot(left, right, preferred_element_type=jnp.float32).astype(jnp.bfloat16)
        out_copy(n).start()
        return carry

    lax.fori_loop(0, S // 2, finish, 0)
    for copy in kv_copies + [x_copy] + kv_forward + wo_own + wo_crossed + halo_pool + halo_kv + [ex_pool, ex_att]:
        copy.wait_send()
    for k in range(2):
        for i in range(len(hops)):
            for copy in z_copies(i, k):
                copy.wait_send()
        for d in range(Z):
            y_copy(d, k).wait_send()
    for n in range(S // 2):
        out_copy(n).wait()


def body(mesh, tokens, norm_gain, w_query, w_key, w_value, w_pool_in, sink_logit, pool_scale, w_out):
    S = lax.axis_size("sp")
    T = lax.axis_size("tp")
    rows, width = tokens.shape
    local_heads = w_query.shape[1] // HEAD
    fits = (
        S % 4 == 0 and S > 4 and T == 2
        and w_out.shape[1] == LANES and w_key.shape[0] == LANES
        and w_query.shape[1] % LANES == 0 and w_pool_in.shape[1] % LANES == 0
        and w_query.shape[1] == w_pool_in.shape[1]
        and local_heads == QH // KVH and rows % (2 * CHUNK) == 0
    )
    if not fits:
        return plain_body(
            tokens, norm_gain, w_query, w_key, w_value, w_pool_in, sink_logit, pool_scale, w_out
        )
    place = lax.axis_index("tp")
    key_head = place * local_heads // (QH // KVH)
    kv_block = jnp.concatenate(
        [
            lax.dynamic_slice_in_dim(w_key, key_head * HEAD, HEAD, 1),
            lax.dynamic_slice_in_dim(w_value, key_head * HEAD, HEAD, 1),
        ],
        axis=1,
    )
    tables = rope_tables(lax.axis_index("sp") * rows, rows)
    blocks = rows // QB
    half = rows // T
    Z = S // 4
    reach = POOL_SPANS[-1] // 2
    wide = w_query.shape[1]
    vmem = pl.BlockSpec(memory_space=pltpu.VMEM)
    smem = pl.BlockSpec(memory_space=pltpu.SMEM)
    hbm = pl.BlockSpec(memory_space=pl.ANY)
    dma = pltpu.SemaphoreType.DMA
    bf = jnp.bfloat16
    return pl.pallas_call(
        functools.partial(mixer_kernel, (S, T)),
        out_shape=jax.ShapeDtypeStruct((half, S * w_out.shape[1]), bf),
        in_specs=[hbm, vmem, hbm, hbm, hbm, smem, vmem, hbm, vmem, vmem, vmem, vmem],
        out_specs=hbm,
        scratch_shapes=[
            pltpu.VMEM((rows, width), bf),
            pltpu.VMEM((rows, width), bf),
            pltpu.VMEM(w_query.shape, bf),
            pltpu.VMEM(w_pool_in.shape, bf),
            pltpu.VMEM((S, LANES, LANES), bf),
            pltpu.VMEM((S, T) + w_out.shape, bf),
            pltpu.VMEM((blocks, local_heads * QB, LANES), bf),
            pltpu.VMEM((rows + 2 * WINDOW, LANES), bf),
            pltpu.VMEM((rows + 2 * reach, wide), jnp.float32),
            pltpu.VMEM((half, wide), bf),
            pltpu.VMEM((half, wide), bf),
            pltpu.VMEM((2 * T, half, wide), bf),
            pltpu.VMEM((S // 2, half, 2 * LANES), bf),
            dma((rows // CHUNK,)),
            dma((4,)),
            dma((S // 2,)),
            dma((S // 2 - 1,)),
            dma((S,)),
            dma((S // 2,)),
            dma(()),
            dma(()),
            dma((T, Z + 1)),
            dma((S, T)),
            dma((T, 2 * (Z - 1))),
            dma((T, Z)),
            dma((4,)),
            dma((4,)),
            dma((2,)),
            dma((2,)),
        ],
        compiler_params=pltpu.CompilerParams(
            collective_id=0, has_side_effects=True, vmem_limit_bytes=62 * 1024 * 1024
        ),
    )(
        tokens, norm_gain[None, :], w_query, kv_block, w_pool_in, sink_logit, pool_scale[None, :], w_out, *tables
    )


def solution(mesh):
    in_specs = (
        P("sp", None),
        P(),
        P(None, "tp"),
        P("sp", None),
        P("sp", None),
        P(None, "tp"),
        P("tp"),
        P("tp"),
        P("tp", "sp"),
    )
    out_specs = P(("sp", "tp"), None)
    return jax.shard_map(functools.partial(body, mesh), mesh=mesh, in_specs=in_specs, out_specs=out_specs, check_vma=False)
```
